512 devices in a mesh: ep: 32 (over z, core), tp: 16 (over y, x).
Axes of the slice: x: 4, y: 4, z: 16, core: 2. Of those that a mesh axis runs over, the one named last changes fastest.
Arguments:
- tokens: bfloat16 [4096, 2048], P('ep'), may hold values from -6 to 6
- routes: int32 [4096, 2], P('ep'), may hold values from 0 to 15, all different within a row; in each aligned block of 128 rows (0 to 127, 128 to 255, ...) at most 18 rows name the same one
- route_weights: float32 [4096, 2], P('ep'), may hold values from 0.2 to 1
- out_grad: bfloat16 [4096, 2048], P('ep'), may hold values from -6 to 6
- gate_proj: bfloat16 [32, 2048, 2048], P('ep', None, 'tp'), may hold values from -0.125 to 0.125
- up_proj: bfloat16 [32, 2048, 2048], P('ep', None, 'tp'), may hold values from -0.125 to 0.125
- down_proj: bfloat16 [32, 2048, 2048], P('ep', 'tp'), may hold values from -0.09375 to 0.09375
Outputs:
- tokens_grad: bfloat16 [4096, 2048], P('ep', 'tp')
- route_grad: float32 [4096, 2], P('ep')
- gate_grad: bfloat16 [32, 2048, 2048], P('ep', None, 'tp')
- up_grad: bfloat16 [32, 2048, 2048], P('ep', None, 'tp')
- down_grad: bfloat16 [32, 2048, 2048], P('ep', 'tp')
The draws below stay inside these ranges and needn't reach their ends.
Inputs may be any that keep to these rules, and one draw needn't show every extreme that they name: `routes`: each row names 2 different experts. In the rows of one device (an aligned block of 128 rows) no expert is named more than 18 times, and in some blocks one expert is named exactly 18 times.
All inputs are finite; a program needn't handle non-finite values.
Results may differ from the reference program's by a relative error of at most 0.019.
Values may be sent and summed in bfloat16 or wider, within the bound.
A program may use at most 64 MiB of HBM per device.

```python
import math
import jax
import jax.numpy as jnp
import numpy as np
from jax import lax

D = 2048
FF = 4096
TOP = 2
TOK_DEV = 128
EXPERTS = 16
SOURCES = 32
GROUPS = 16
HALF = 2048
CAP = 18
ROWS = 576
TOKENS = 4096


def steps_of(rng, shape, pieces, low, largest):
    factor_of, own = 1.0, jax.random.fold_in(rng, 6)
    for dim, blocks in pieces:
        draws = jnp.exp(jax.random.uniform(jax.random.fold_in(own, dim), (blocks,), jnp.float32, low / len(pieces), largest / len(pieces)))
        factor_of = factor_of * jnp.repeat(draws, shape[dim] // blocks).reshape([-1 if axis == dim else 1 for axis in range(len(shape))])
    return factor_of


def shared_out(key, own, number, rows, number_of, top, limit, lean):
    ranking = jax.random.permutation(key, number_of)
    crowded, ordinary = portions_of(number_of, rows * top, limit, lean, True), portions_of(number_of, rows * top, limit, lean, False)
    places = jnp.arange(number_of)

    def named(tallies, rotation):
        used = int((tallies > 0).sum())
        fixed = max(1, used // 4)
        passed = fixed + (places - fixed + rotation * (used - fixed)) % max(1, number_of - fixed)
        return jnp.zeros((number_of,), jnp.int32).at[ranking[jnp.where(places < fixed, places, passed)]].set(jnp.asarray(tallies, jnp.int32))

    tallies = jnp.where(number % 4 == 0, named(crowded, number // 4), named(ordinary, number - number // 4 - 1))
    mixed = jax.random.permutation(jax.random.fold_in(own, 3), number_of)
    source_of, taker = mixed[0:number_of // 2 * 2:2], mixed[1:number_of // 2 * 2:2]
    slack = jnp.minimum(tallies[source_of] - 1, limit - tallies[taker]) // 2
    slack = jnp.where((source_of == ranking[0]) | (taker == ranking[0]) | (tallies[taker] == 0), 0, jnp.maximum(slack, 0))
    passed = jax.random.randint(jax.random.fold_in(own, 4), (number_of // 2,), 0, 1 << 20) % (slack + 1)
    tallies = tallies.at[source_of].add(-passed).at[taker].add(passed)
    members = jnp.searchsorted(jnp.cumsum(tallies), jnp.arange(rows * top), side="right").astype(jnp.int32)
    listing = members.reshape(top, rows).T
    listing = listing[jax.random.permutation(jax.random.fold_in(own, 1), rows)]
    rotation = jax.random.randint(jax.random.fold_in(own, 2), (rows, 1), 0, top)
    return jnp.take_along_axis(listing, (jnp.arange(top)[None, :] + rotation) % top, axis=1)


def portions_of(number_of, total, most, lean, full):
    portions = [(1 << 20) // math.isqrt(standing ** lean) + 1 for standing in range(1, number_of + 1)]
    largest = most if full else min(most, max(-(-total // number_of), total * portions[0] // sum(portions)))
    least = 1 if total - largest >= number_of - 1 else 0
    holding, rest = [largest] + [least] * (number_of - 1), total - largest - least * (number_of - 1)
    while rest > 0:
        free = [i for i in range(1, number_of) if holding[i] < largest] or [i for i in range(1, number_of) if holding[i] < most]
        whole, remaining = sum([portions[i] for i in free]), rest
        for i in free:
            more = min(most - holding[i], max(1, remaining * portions[i] // whole), rest)
            holding[i] = holding[i] + more
            rest = rest - more
    return np.array(holding)


def gaussian(rng, extent, spread, most, split=(), kind=jnp.bfloat16):
    array = spread * jax.random.normal(rng, extent, jnp.float32)
    if split:
        array = array * steps_of(rng, extent, split, -0.22, 0.18)
    return jnp.clip(array, -most, most).astype(kind)


def setup_inputs(seed: int = 0) -> dict:
    seeds = jax.random.split(jax.random.key(seed), 8)
    tokens = gaussian(seeds[0], (TOKENS, D), 1.0, 6.0, ((0, 32),))
    routes_keys = jax.random.split(jax.random.fold_in(seeds[1], 1), TOKENS // TOK_DEV)
    routes_turns = jax.random.permutation(jax.random.fold_in(seeds[1], 3), TOKENS // TOK_DEV)
    routes = jax.vmap(lambda own, number: shared_out(jax.random.fold_in(seeds[1], 2), own, number, TOK_DEV, EXPERTS, TOP, CAP, 2))(routes_keys, routes_turns).reshape((TOKENS, TOP))
    route_weights = jnp.clip(0.2 + 0.8 * jax.random.uniform(seeds[2], (TOKENS, TOP), jnp.float32) ** steps_of(seeds[2], (TOKENS, TOP), ((0, 32),), -0.2, 0.2), 0.2, 1.0)
    out_grad = gaussian(seeds[3], (TOKENS, D), 1.0, 6.0, ((0, 32),))
    gate_proj = gaussian(seeds[4], (2 * EXPERTS, D, HALF), D ** -0.5, 0.125, ((0, 32), (2, 16)))
    up_proj = gaussian(seeds[5], (2 * EXPERTS, D, HALF), D ** -0.5, 0.125, ((0, 32), (2, 16)))
    down_proj = gaussian(seeds[6], (2 * EXPERTS, HALF, D), FF ** -0.5, 0.09375, ((0, 32), (1, 16)))
    return dict(tokens=tokens, routes=routes, route_weights=route_weights, out_grad=out_grad, gate_proj=gate_proj, up_proj=up_proj, down_proj=down_proj)


def slot_rows(routes):
    blocks = routes.reshape(SOURCES, TOK_DEV * TOP)
    one_hot = (blocks[:, :, None] == jnp.arange(EXPERTS, dtype=jnp.int32)[None, None, :]).astype(jnp.int32)
    earlier = jnp.cumsum(one_hot, axis=1) - one_hot
    slot_index = jnp.sum(earlier * one_hot, axis=2)
    source = jnp.arange(SOURCES, dtype=jnp.int32)[:, None]
    return (blocks * ROWS + source * CAP + slot_index).reshape(-1).astype(jnp.int32)


def contract_rows(left, right):
    return lax.dot_general(left, right, (((0,), (0,)), ((), ())), preferred_element_type=jnp.float32)


def reference(tokens, routes, route_weights, out_grad, gate_proj, up_proj, down_proj):
    position = slot_rows(routes)
    owner = (jnp.arange(TOKENS * TOP, dtype=jnp.int32) // TOP).astype(jnp.int32)
    all_rows = EXPERTS * ROWS
    x_all = jnp.zeros((all_rows, D), jnp.bfloat16).at[position].set(tokens[owner]).reshape(EXPERTS, ROWS, D)
    dy_all = jnp.zeros((all_rows, D), jnp.bfloat16).at[position].set(out_grad[owner]).reshape(EXPERTS, ROWS, D)
    g_all = jnp.zeros((all_rows,), jnp.float32).at[position].set(route_weights.reshape(-1)).reshape(EXPERTS, ROWS)
    group_width = HALF // GROUPS

    def one_half(index):
        expert = index // 2
        x_rows = x_all[expert]
        dy_rows = dy_all[expert]
        g_rows = g_all[expert][:, None]
        gate_w = gate_proj[index]
        up_w = up_proj[index]
        down_w = down_proj[index]
        pre_gate = jnp.dot(x_rows, gate_w, preferred_element_type=jnp.float32)
        pre_up = jnp.dot(x_rows, up_w, preferred_element_type=jnp.float32)
        sigma = jax.nn.sigmoid(pre_gate)
        activ = pre_gate * sigma
        hidden = activ * pre_up
        d_hidden = lax.dot_general(dy_rows, down_w, (((1,), (1,)), ((), ())), preferred_element_type=jnp.float32)
        gate_part = jnp.sum(hidden * d_hidden, axis=1)
        scaled = g_rows * d_hidden
        d_gate = (scaled * pre_up * sigma * (1.0 + pre_gate * (1.0 - sigma))).astype(jnp.bfloat16)
        d_up = (scaled * activ).astype(jnp.bfloat16)
        scaled_cot = (g_rows * dy_rows.astype(jnp.float32)).astype(jnp.bfloat16)
        grad_gate = contract_rows(x_rows, d_gate).astype(jnp.bfloat16)
        grad_up = contract_rows(x_rows, d_up).astype(jnp.bfloat16)
        grad_down = contract_rows(hidden.astype(jnp.bfloat16), scaled_cot).astype(jnp.bfloat16)
        gate_three = d_gate.astype(jnp.float32).reshape(ROWS, GROUPS, group_width)
        up_three = d_up.astype(jnp.float32).reshape(ROWS, GROUPS, group_width)
        gate_wide = gate_w.astype(jnp.float32).reshape(D, GROUPS, group_width)
        up_wide = up_w.astype(jnp.float32).reshape(D, GROUPS, group_width)
        partial_value = jnp.einsum("rqc,dqc->qrd", gate_three, gate_wide, precision=lax.Precision.HIGHEST)
        partial_value = partial_value + jnp.einsum("rqc,dqc->qrd", up_three, up_wide, precision=lax.Precision.HIGHEST)
        rounded = lax.optimization_barrier(partial_value.astype(jnp.bfloat16)).astype(jnp.float32)
        row_grad = jnp.sum(rounded, axis=0).astype(jnp.bfloat16)
        return row_grad, gate_part, grad_gate, grad_up, grad_down

    row_grad, gate_part, gate_grad, up_grad, down_grad = lax.map(one_half, jnp.arange(2 * EXPERTS, dtype=jnp.int32))
    expert_rows = row_grad.astype(jnp.float32).reshape(EXPERTS, 2, ROWS, D).sum(axis=1).reshape(all_rows, D)
    expert_gate = gate_part.reshape(EXPERTS, 2, ROWS).sum(axis=1).reshape(all_rows)
    tokens_grad = expert_rows[position].reshape(TOKENS, TOP, D).sum(axis=1).astype(jnp.bfloat16)
    route_grad = expert_gate[position].reshape(TOKENS, TOP)
    return (tokens_grad, route_grad, gate_grad, up_grad, down_grad)
```

```python
import jax
import jax.numpy as jnp
from jax import lax
from jax.experimental import pallas as pl
from jax.experimental.pallas import tpu as pltpu
from jax.sharding import PartitionSpec as P

MESH = pl.DeviceIdType.MESH
F32, BF16 = jnp.float32, jnp.bfloat16
NZ, SIDE = 16, 4
CAP, PAD = 18, 32
LANES = 128
MODEL = 2048
HALF_ROWS = NZ * CAP
ROWS = 2 * HALF_ROWS
QUARTER = HALF_ROWS // 2
HIGHEST = lax.Precision.HIGHEST


def dot(left, right, dims, precision=None):
    return lax.dot_general(
        left, right, ((dims[:1], dims[1:]), ((), ())), precision=precision,
        preferred_element_type=F32,
    )


def far_first(i):
    step = (i + 1) // 2
    return NZ // 2 + step * (1 - 2 * (i % 2))


def kernel(
    routes, weights, tok_hbm, cot_hbm, gate_hbm, up_hbm, down_hbm,
    out_tok, out_route, out_gate, out_up, out_down,
    tok_v, cot_v, wgu, down_v, pall, send, recv, pad, xs, dgu, hid, prod,
    dother, crecv, dacc, rs, r1, r2, send2, q1, q2, fin, ret, home,
    g0, g1, g2, ga, gb, gc, gs, gr, og, ou, od,
    in_sem, out_sem, z_send, z_recv, s1, n1, s2, n2, ps, pn,
    cs, cn, rs_send, rs_recv, qs, qn, fs, fn, gas, gan, gbs, gbn, gcs, gcn, gzs, gzn,
):
    ep, t = lax.axis_index("ep"), lax.axis_index("tp")
    z, c = ep // 2, ep % 2
    y, x = t // SIDE, t % SIDE
    p1, p2 = x + c * (y - x), y + c * (x - y)
    w1, w2 = 1 + 3 * c, 4 - 3 * c

    def block(o1, o2):
        return w1 * ((p1 + o1) % SIDE) + w2 * ((p2 + o2) % SIDE)

    def block_of_partner(o1, o2):
        return w2 * ((p2 + o1) % SIDE) + w1 * ((p1 + o2) % SIDE)

    def along1(o):
        return (ep, block(o, 0))

    def along2(o):
        return (ep, block(0, o))

    partner = (z * 2 + 1 - c, t)

    def remote(src, dst, send_sem, recv_sem, device):
        return pltpu.make_async_remote_copy(
            src_ref=src, dst_ref=dst, send_sem=send_sem, recv_sem=recv_sem,
            device_id=device, device_id_type=MESH,
        )

    barrier = pltpu.get_barrier_semaphore()

    def greet(i, carry):
        pl.semaphore_signal(barrier, inc=1, device_id=((ep + i) % (2 * NZ), t), device_id_type=MESH)
        return carry

    lax.fori_loop(1, 2 * NZ, greet, 0)
    for o in range(1, SIDE):
        pl.semaphore_signal(barrier, inc=1, device_id=along1(o), device_id_type=MESH)
        pl.semaphore_signal(barrier, inc=1, device_id=along2(o), device_id_type=MESH)

    own_cols = pl.ds(pl.multiple_of(t * LANES, LANES), LANES)
    loads = [
        pltpu.make_async_copy(tok_hbm.at[:, own_cols], tok_v, in_sem.at[0]),
        pltpu.make_async_copy(cot_hbm.at[:, own_cols], cot_v, in_sem.at[1]),
        pltpu.make_async_copy(gate_hbm.at[0], wgu.at[:, pl.ds(0, LANES)], in_sem.at[2]),
        pltpu.make_async_copy(up_hbm.at[0], wgu.at[:, pl.ds(LANES, LANES)], in_sem.at[3]),
        pltpu.make_async_copy(down_hbm.at[0], down_v, in_sem.at[4]),
    ]
    for load in loads:
        load.start()

    r0, r1_ = routes[0:1, :], routes[1:2, :]
    experts = lax.broadcasted_iota(jnp.int32, (NZ, LANES), 0)
    hit0, hit1 = experts == r0, experts == r1_
    named = jnp.logical_or(hit0, hit1)
    earlier_than = (
        lax.broadcasted_iota(jnp.int32, (LANES, LANES), 0)
        < lax.broadcasted_iota(jnp.int32, (LANES, LANES), 1)
    ).astype(BF16)
    earlier = dot(named.astype(F32).astype(BF16), earlier_than, (1, 0))
    place = jnp.where(named, earlier, -1.0)
    weight = jnp.where(hit0, weights[0:1, :], 0.0) + jnp.where(hit1, weights[1:2, :], 0.0)
    slot_ids = lax.broadcasted_iota(jnp.int32, (PAD, LANES), 0).astype(F32)
    gains = []
    for e in range(NZ):
        picked = slot_ids == place[e : e + 1, :]
        pall[PAD * e : PAD * (e + 1), :] = picked.astype(F32).astype(BF16)
        gains.append(
            jnp.sum(jnp.where(picked, weight[e : e + 1, :], 0.0), axis=1, keepdims=True)
        )
    pad[...] = jnp.zeros_like(pad)
    home[...] = jnp.zeros_like(home)
    loads[0].wait()
    rows = dot(pall[...], tok_v[...], (1, 0)).astype(BF16)
    for e in range(NZ):
        send[0, e] = rows[PAD * e : PAD * e + CAP, :]
    loads[1].wait()
    rows = dot(pall[...], cot_v[...], (1, 0))
    for e in range(NZ):
        send[1, e] = (rows[PAD * e : PAD * e + CAP, :] * gains[e][:CAP, :]).astype(BF16)
    squeeze_r = lax.broadcasted_iota(jnp.int32, (QUARTER, 8 * PAD), 0)
    squeeze_p = lax.broadcasted_iota(jnp.int32, (QUARTER, 8 * PAD), 1)
    slot = squeeze_p % PAD
    squeeze = jnp.logical_and(
        squeeze_r == (squeeze_p // PAD) * CAP + slot, slot < CAP
    ).astype(F32)
    squeeze_b = squeeze.astype(BF16)

    pl.semaphore_wait(barrier, 2 * NZ - 1 + 2 * (SIDE - 1))

    def to_same(dz):
        i = c * NZ + dz
        to = (z + dz) % NZ
        return remote(send.at[c, to], recv.at[i], z_send.at[0, dz], z_recv.at[i], (to * 2 + c, t))

    def to_other(dz):
        i = c * NZ + dz
        to = (z + dz) % NZ
        return remote(
            send.at[1 - c, to], recv.at[i], z_send.at[1, dz], z_recv.at[i], (to * 2 + 1 - c, t)
        )

    def dispatch(i, carry):
        dz = far_first(i)
        to_same(dz).start()
        to_other(dz).start()
        return carry

    lax.fori_loop(0, NZ - 1, dispatch, 0)
    to_other(0).start()
    recv[c * NZ] = send[c, z]

    def arrived(i):
        remote(recv.at[i], recv.at[i], z_send.at[0, 0], z_recv.at[i], partner).wait_recv()

    arrived((1 - c) * NZ)

    def arrive(dz, carry):
        arrived(dz)
        arrived(NZ + dz)
        return carry

    lax.fori_loop(1, NZ, arrive, 0)
    for i in range(2 * NZ):
        pad[PAD * i : PAD * i + CAP, :] = recv[i]
    for k in range(4):
        xs[c, QUARTER * k : QUARTER * (k + 1), own_cols] = dot(
            squeeze_b, pad[8 * PAD * k : 8 * PAD * (k + 1), :], (1, 0)
        ).astype(BF16)

    waits = []

    def piece(o1, o2, first, count):
        cols = pl.ds(pl.multiple_of(block(o1, o2) * LANES, LANES), LANES)
        return xs.at[c, pl.ds(first, count), cols]

    WHOLE, LOW, HIGH = (0, ROWS), (0, HALF_ROWS), (HALF_ROWS, HALF_ROWS)

    def pass_on(o1, o2, part, send_sem, recv_sem, device):
        ref = piece(o1, o2, *part)
        copy = remote(ref, ref, send_sem, recv_sem, device)
        copy.start()
        waits.append(copy)

    def came(o1, o2, part, recv_sem):
        ref = piece(o1, o2, *part)
        remote(ref, ref, recv_sem, recv_sem, partner).wait_recv()

    def hand_over(o1, o2):
        i = (o1 % SIDE) * SIDE + o2 % SIDE
        pass_on(o1, o2, WHOLE, ps.at[i], pn.at[i], partner)

    def both_ways(o1):
        j = o1 % SIDE
        pass_on(o1, 0, WHOLE, s2.at[j, 0], n2.at[j, 0], along2(1))
        pass_on(o1, 0, WHOLE, s2.at[j, 1], n2.at[j, 1], along2(-1))

    pass_on(0, 0, WHOLE, s1.at[0], n1.at[0], along1(1))
    pass_on(0, 0, WHOLE, s1.at[1], n1.at[1], along1(-1))
    both_ways(0)
    hand_over(0, 0)
    came(-1, 0, WHOLE, n1.at[0])
    pass_on(-1, 0, LOW, s1.at[2], n1.at[2], along1(1))
    both_ways(-1)
    hand_over(-1, 0)
    came(1, 0, WHOLE, n1.at[1])
    pass_on(1, 0, HIGH, s1.at[3], n1.at[3], along1(-1))
    both_ways(1)
    hand_over(1, 0)

    def across(o1):
        j = o1 % SIDE
        came(o1, -1, WHOLE, n2.at[j, 0])
        pass_on(o1, -1, LOW, s2.at[j, 2], n2.at[j, 2], along2(1))
        hand_over(o1, -1)
        came(o1, 1, WHOLE, n2.at[j, 1])
        pass_on(o1, 1, HIGH, s2.at[j, 3], n2.at[j, 3], along2(-1))
        hand_over(o1, 1)

    across(0)
    came(2, 0, LOW, n1.at[2])
    came(2, 0, HIGH, n1.at[3])
    both_ways(2)
    hand_over(2, 0)
    for o1 in (-1, 1, 2):
        across(o1)
    for o1 in (0, -1, 1, 2):
        j = o1 % SIDE
        came(o1, 2, LOW, n2.at[j, 2])
        came(o1, 2, HIGH, n2.at[j, 3])
        hand_over(o1, 2)
    for o1 in range(SIDE):
        for o2 in range(SIDE):
            cols = pl.ds(pl.multiple_of(block_of_partner(o1, o2) * LANES, LANES), LANES)
            ref = xs.at[1 - c, :, cols]
            remote(ref, ref, pn.at[o1 * SIDE + o2], pn.at[o1 * SIDE + o2], partner).wait_recv()

    for load in loads[2:]:
        load.wait()
    pre = dot(xs[0], wgu[...], (1, 0))
    dh = dot(xs[1], down_v[...], (1, 1))
    a, b = pre[:, :LANES], pre[:, LANES:]
    sigma = jax.nn.sigmoid(a)
    activ = a * sigma
    hidden = activ * b
    dgu[:, :LANES] = (dh * b * sigma * (1.0 + a * (1.0 - sigma))).astype(BF16)
    dgu[:, LANES:] = (dh * activ).astype(BF16)
    hid[...] = hidden.astype(BF16)
    prod[...] = hidden * dh

    others = pl.ds(pl.multiple_of((1 - c) * HALF_ROWS, HALF_ROWS), HALF_ROWS)
    owns = pl.ds(pl.multiple_of(c * HALF_ROWS, HALF_ROWS), HALF_ROWS)
    order = (2, 1, 3, 0)
    combine = {}
    for o1 in order:
        for o2 in range(SIDE):
            wrows = pl.ds(pl.multiple_of(block_of_partner(o1, o2) * LANES, LANES), LANES)
            dother[o1, o2] = dot(dgu[others, :], wgu[wrows, :], (1, 1)).astype(BF16)
        combine[o1] = remote(dother.at[o1], crecv.at[o1], cs.at[o1], cn.at[o1], partner)
        combine[o1].start()
    waits.extend(combine.values())
    for o1 in order:
        for o2 in range(SIDE):
            wrows = pl.ds(pl.multiple_of(block(o1, o2) * LANES, LANES), LANES)
            dacc[o1, o2] = dot(dgu[owns, :], wgu[wrows, :], (1, 1))

    lo, hi = pl.ds(0, QUARTER), pl.ds(QUARTER, QUARTER)

    def ship(src, dst, send_sem, recv_sem, device):
        copy = remote(src, dst, send_sem, recv_sem, device)
        copy.start()
        waits.append(copy)
        return copy

    combine[2].wait_recv()
    rs[2] = (dacc[2] + crecv[2].astype(F32)).astype(BF16)
    first_up = ship(rs.at[2, :, lo], r1.at[0], rs_send.at[0], rs_recv.at[0], along1(1))
    first_down = ship(rs.at[2, :, hi], r1.at[1], rs_send.at[1], rs_recv.at[1], along1(-1))
    combine[1].wait_recv()
    rs[1, :, hi] = (dacc[1, :, hi] + crecv[1, :, hi].astype(F32)).astype(BF16)
    up_hi = ship(rs.at[1, :, hi], r2.at[0, :, hi], rs_send.at[2], rs_recv.at[2], along1(1))
    combine[3].wait_recv()
    rs[3, :, lo] = (dacc[3, :, lo] + crecv[3, :, lo].astype(F32)).astype(BF16)
    down_lo = ship(rs.at[3, :, lo], r2.at[1, :, lo], rs_send.at[3], rs_recv.at[3], along1(-1))
    first_up.wait_recv()
    rs[1, :, lo] = (
        dacc[1, :, lo] + crecv[1, :, lo].astype(F32) + r1[0].astype(F32)
    ).astype(BF16)
    up_lo = ship(rs.at[1, :, lo], r2.at[0, :, lo], rs_send.at[4], rs_recv.at[4], along1(1))
    first_down.wait_recv()
    rs[3, :, hi] = (
        dacc[3, :, hi] + crecv[3, :, hi].astype(F32) + r1[1].astype(F32)
    ).astype(BF16)
    down_hi = ship(rs.at[3, :, hi], r2.at[1, :, hi], rs_send.at[5], rs_recv.at[5], along1(-1))

    for k in range(4):
        spread = dot(squeeze, prod[QUARTER * k : QUARTER * (k + 1), :], (0, 0), HIGHEST)
        g0[:, 8 * PAD * k : 8 * PAD * (k + 1)] = dot(
            jnp.ones((8, LANES), F32), spread, (1, 1), HIGHEST
        )
    first = [ship(g0, ga.at[o - 1], gas.at[o - 1], gan.at[o - 1], along1(o)) for o in (1, 2, 3)]

    def grads(k, carry):
        cols = pl.ds(pl.multiple_of(k * 256, 256), 256)
        part = dot(xs[0, :, cols], dgu[...], (0, 0))
        og[cols, :] = part[:, :LANES].astype(BF16)
        ou[cols, :] = part[:, LANES:].astype(BF16)
        return carry

    lax.fori_loop(0, MODEL // 256, grads, 0)
    stores = [
        pltpu.make_async_copy(og, out_gate.at[0], out_sem.at[0]),
        pltpu.make_async_copy(ou, out_up.at[0], out_sem.at[1]),
        pltpu.make_async_copy(od, out_down.at[0], out_sem.at[2]),
    ]
    stores[0].start()
    stores[1].start()
    for copy in first:
        copy.wait_recv()
    g1[...] = g0[...] + ga[0] + ga[1] + ga[2]
    second = [ship(g1, gb.at[o - 1], gbs.at[o - 1], gbn.at[o - 1], along2(o)) for o in (1, 2, 3)]

    combine[0].wait_recv()
    for copy in (up_hi, down_lo, up_lo, down_hi):
        copy.wait_recv()
    for o2 in (2, 1, 3, 0):
        dacc[0, o2] = (
            dacc[0, o2] + crecv[0, o2].astype(F32) + r2[0, o2].astype(F32) + r2[1, o2].astype(F32)
        )
        if o2:
            send2[o2] = dacc[0, o2].astype(BF16)
        if o2 == 2:
            first_up = ship(send2.at[2, lo], q1.at[0], qs.at[0], qn.at[0], along2(1))
            first_down = ship(send2.at[2, hi], q1.at[1], qs.at[1], qn.at[1], along2(-1))
        if o2 == 1:
            up_hi = ship(send2.at[1, hi], q2.at[0, hi], qs.at[2], qn.at[2], along2(1))
        if o2 == 3:
            down_lo = ship(send2.at[3, lo], q2.at[1, lo], qs.at[3], qn.at[3], along2(-1))
    for copy in second:
        copy.wait_recv()
    g2[...] = g1[...] + gb[0] + gb[1] + gb[2]
    third = ship(g2, gc, gcs.at[0], gcn.at[0], partner)
    first_up.wait_recv()
    send2[0, lo] = (dacc[0, 1, lo] + q1[0].astype(F32)).astype(BF16)
    up_lo = ship(send2.at[0, lo], q2.at[0, lo], qs.at[4], qn.at[4], along2(1))
    first_down.wait_recv()
    send2[0, hi] = (dacc[0, 3, hi] + q1[1].astype(F32)).astype(BF16)
    down_hi = ship(send2.at[0, hi], q2.at[1, hi], qs.at[5], qn.at[5], along2(-1))
    third.wait_recv()
    lanes = pl.ds(pl.multiple_of(c * NZ * PAD, NZ * PAD), NZ * PAD)
    spread = dot(
        g2[:, lanes] + gc[:, lanes], jnp.full((8, LANES), 0.125, F32), (0, 0), HIGHEST
    )
    for i in range(NZ):
        gs[i] = spread[PAD * i : PAD * i + CAP, :]

    def gate_home(dz):
        return remote(gs.at[dz], gr.at[dz], gzs.at[dz], gzn.at[dz], ((z - dz) % NZ * 2 + c, t))

    def send_gate(i, carry):
        gate_home(far_first(i)).start()
        return carry

    lax.fori_loop(0, NZ - 1, send_gate, 0)
    gr[0] = gs[0]
    for copy in (up_hi, down_lo, up_lo, down_hi):
        copy.wait_recv()
    total = (dacc[0, 0] + q2[0].astype(F32) + q2[1].astype(F32)).astype(BF16)
    for k in range(2):
        spread = dot(squeeze_b, total[QUARTER * k : QUARTER * (k + 1), :], (0, 0)).astype(BF16)
        for i in range(8):
            fin[8 * k + i] = spread[PAD * i : PAD * i + CAP, :]

    def rows_home(dz):
        return remote(fin.at[dz], ret.at[dz], fs.at[dz], fn.at[dz], ((z - dz) % NZ * 2 + c, t))

    def send_rows(i, carry):
        rows_home(far_first(i)).start()
        return carry

    lax.fori_loop(0, NZ - 1, send_rows, 0)
    ret[0] = fin[0]
    od[...] = dot(hid[...], xs[1], (0, 0)).astype(BF16)
    stores[2].start()

    def gates_came(dz, carry):
        gate_home(dz).wait_recv()
        return carry

    lax.fori_loop(1, NZ, gates_came, 0)

    def add_gates(dz, carry):
        e = (z + dz) % NZ
        at = pl.ds(pl.multiple_of(e * PAD, PAD), PAD)
        v = jnp.sum(gr[dz] * pall[at, :][:CAP, :].astype(F32), axis=0, keepdims=True)
        return (carry[0] + jnp.where(r0 == e, v, 0.0), carry[1] + jnp.where(r1_ == e, v, 0.0))

    zero = jnp.zeros((1, LANES), F32)
    v0, v1 = lax.fori_loop(0, NZ, add_gates, (zero, zero))
    out_route[0:1, :] = v0 / weights[0:1, :]
    out_route[1:2, :] = v1 / weights[1:2, :]

    def rows_came(dz, carry):
        rows_home(dz).wait_recv()
        return carry

    lax.fori_loop(1, NZ, rows_came, 0)

    def put_home(dz, carry):
        e = (z + dz) % NZ
        home[e, :CAP, :] = ret[dz]
        return carry

    lax.fori_loop(0, NZ, put_home, 0)
    out_tok[...] = dot(pall[...], home[...].reshape(NZ * PAD, LANES), (0, 0)).astype(BF16)

    def drain(dz, carry):
        to_same(dz).wait_send()
        to_other(dz).wait_send()
        gate_home(dz).wait_send()
        rows_home(dz).wait_send()
        return carry

    lax.fori_loop(1, NZ, drain, 0)
    to_other(0).wait_send()
    for copy in waits:
        copy.wait_send()
    for store in stores:
        store.wait()


def local(tokens, routes, route_weights, out_grad, gate_proj, up_proj, down_proj):
    vmem, hbm = pl.BlockSpec(memory_space=pltpu.VMEM), pl.BlockSpec(memory_space=pl.ANY)
    dma, buf = pltpu.SemaphoreType.DMA, pltpu.VMEM
    quad = (SIDE, HALF_ROWS, LANES)
    out = pl.pallas_call(
        kernel,
        out_shape=(
            jax.ShapeDtypeStruct((LANES, LANES), BF16),
            jax.ShapeDtypeStruct((2, LANES), F32),
            jax.ShapeDtypeStruct((1, MODEL, LANES), BF16),
            jax.ShapeDtypeStruct((1, MODEL, LANES), BF16),
            jax.ShapeDtypeStruct((1, LANES, MODEL), BF16),
        ),
        in_specs=[vmem, vmem, hbm, hbm, hbm, hbm, hbm],
        out_specs=[vmem, vmem, hbm, hbm, hbm],
        scratch_shapes=[
            buf((LANES, LANES), BF16),
            buf((LANES, LANES), BF16),
            buf((MODEL, 2 * LANES), BF16),
            buf((LANES, MODEL), BF16),
            buf((NZ * PAD, LANES), BF16),
            buf((2, NZ, CAP, LANES), BF16),
            buf((2 * NZ, CAP, LANES), BF16),
            buf((2 * NZ * PAD, LANES), BF16),
            buf((2, ROWS, MODEL), BF16),
            buf((ROWS, 2 * LANES), BF16),
            buf((ROWS, LANES), BF16),
            buf((ROWS, LANES), F32),
            buf((SIDE, *quad), BF16),
            buf((SIDE, *quad), BF16),
            buf((SIDE, *quad), F32),
            buf((SIDE, *quad), BF16),
            buf((2, SIDE, QUARTER, LANES), BF16),
            buf((2, *quad), BF16),
            buf(quad, BF16),
            buf((2, QUARTER, LANES), BF16),
            buf((2, HALF_ROWS, LANES), BF16),
            buf((NZ, CAP, LANES), BF16),
            buf((NZ, CAP, LANES), BF16),
            buf((NZ, PAD, LANES), BF16),
            buf((8, 2 * NZ * PAD), F32),
            buf((8, 2 * NZ * PAD), F32),
            buf((8, 2 * NZ * PAD), F32),
            buf((3, 8, 2 * NZ * PAD), F32),
            buf((3, 8, 2 * NZ * PAD), F32),
            buf((8, 2 * NZ * PAD), F32),
            buf((NZ, CAP, LANES), F32),
            buf((NZ, CAP, LANES), F32),
            buf((MODEL, LANES), BF16),
            buf((MODEL, LANES), BF16),
            buf((LANES, MODEL), BF16),
            dma((5,)),
            dma((3,)),
            dma((2, NZ)),
            dma((2 * NZ,)),
            dma((4,)),
            dma((4,)),
            dma((SIDE, 4)),
            dma((SIDE, 4)),
            dma((SIDE * SIDE,)),
            dma((SIDE * SIDE,)),
            dma((SIDE,)),
            dma((SIDE,)),
            dma((6,)),
            dma((6,)),
            dma((6,)),
            dma((6,)),
            dma((NZ,)),
            dma((NZ,)),
            dma((3,)),
            dma((3,)),
            dma((3,)),
            dma((3,)),
            dma((1,)),
            dma((1,)),
            dma((NZ,)),
            dma((NZ,)),
        ],
        compiler_params=pltpu.CompilerParams(
            collective_id=0, has_side_effects=True, vmem_limit_bytes=56 * 2**20
        ),
        name="routed_backward",
    )(routes.T, route_weights.T, tokens, out_grad, gate_proj, up_proj, down_proj)
    return (out[0], out[1].T, out[2], out[3], out[4])


def solution(mesh):
    placed = (
        P("ep", None),
        P("ep", None),
        P("ep", None),
        P("ep", None),
        P("ep", None, "tp"),
        P("ep", None, "tp"),
        P("ep", "tp", None),
    )
    return jax.shard_map(
        local,
        mesh=mesh,
        in_specs=placed,
        out_specs=(
            P("ep", "tp"),
            P("ep", None),
            P("ep", None, "tp"),
            P("ep", None, "tp"),
            P("ep", "tp", None),
        ),
        check_vma=False,
    )
```

```python
import jax
import jax.numpy as jnp
from jax import lax
from jax.experimental import pallas as pl
from jax.experimental.pallas import tpu as pltpu
from jax.sharding import PartitionSpec as P

MESH = pl.DeviceIdType.MESH
F32, BF16 = jnp.float32, jnp.bfloat16
NZ, SIDE = 16, 4
CAP, PAD, BACK = 18, 32, 20
LANES = 128
MODEL = 2048
ROWS = 2 * NZ * CAP
CHUNKS = 1
NEAR = NZ // CHUNKS
HALF = NEAR * CAP
PART = 2 * HALF
CUT = (HALF // 2 + 7) // 8 * 8
SELF, OTHERS = NZ - 1, (0, NZ - 1)
GATES = NEAR * PAD // LANES


def dot(left, right, dims):
    return lax.dot_general(
        left, right, ((dims[:1], dims[1:]), ((), ())), preferred_element_type=F32
    )


def away(i):
    step = NZ // 2 - (i + 1) // 2
    return step * (2 * (i % 2) - 1)


def kernel(
    routes, weights, tok_hbm, cot_hbm, gate_hbm, up_hbm, down_hbm,
    out_tok, out_route, og, ou, od,
    tok_v, cot_v, wgu, down_v, pall, send, recv, pad, xs, dgu, hid,
    dother, crecv, dacc, rs, r1, r2, send2, q1, q2, fin, ret, home, gp, gq, gsum, gall, gt,
    in_sem, z_send, z_recv, s1, n1, s2, n2, ps, pn,
    cs, cn, rs_send, rs_recv, qs, qn, fs, fn, gs, gn, hs, hn,
):
    ep, t = lax.axis_index("ep"), lax.axis_index("tp")
    z, c = ep // 2, ep % 2
    y, x = t // SIDE, t % SIDE
    p1, p2 = x + c * (y - x), y + c * (x - y)
    w1, w2 = 1 + 3 * c, 4 - 3 * c

    def block(o1, o2):
        return w1 * ((p1 + o1) % SIDE) + w2 * ((p2 + o2) % SIDE)

    def block_of_partner(o1, o2):
        return w2 * ((p2 + o1) % SIDE) + w1 * ((p1 + o2) % SIDE)

    def along1(o):
        return (ep, block(o, 0))

    def along2(o):
        return (ep, block(0, o))

    partner = (z * 2 + 1 - c, t)

    def remote(src, dst, send_sem, recv_sem, device):
        return pltpu.make_async_remote_copy(
            src_ref=src, dst_ref=dst, send_sem=send_sem, recv_sem=recv_sem,
            device_id=device, device_id_type=MESH,
        )

    scope = []

    def phase(name):
        if scope:
            scope.pop().__exit__(None, None, None)
        if name:
            scope.append(jax.named_scope(name))
            scope[0].__enter__()

    phase("greet")
    barrier = pltpu.get_barrier_semaphore()

    def greet(i, carry):
        pl.semaphore_signal(barrier, inc=1, device_id=((ep + i) % (2 * NZ), t), device_id_type=MESH)
        return carry

    def greet_plane(i, carry):
        to = (ep, (t + i) % (SIDE * SIDE))
        pl.semaphore_signal(barrier, inc=1, device_id=to, device_id_type=MESH)
        return carry

    lax.fori_loop(1, 2 * NZ, greet, 0)
    lax.fori_loop(1, SIDE * SIDE, greet_plane, 0)

    own_cols = pl.ds(pl.multiple_of(t * LANES, LANES), LANES)
    loads = [
        pltpu.make_async_copy(tok_hbm.at[:, own_cols], tok_v, in_sem.at[0]),
        pltpu.make_async_copy(cot_hbm.at[:, own_cols], cot_v, in_sem.at[1]),
        pltpu.make_async_copy(gate_hbm.at[0], wgu.at[:, pl.ds(0, LANES)], in_sem.at[2]),
        pltpu.make_async_copy(up_hbm.at[0], wgu.at[:, pl.ds(LANES, LANES)], in_sem.at[3]),
        pltpu.make_async_copy(down_hbm.at[0], down_v, in_sem.at[4]),
    ]
    for load in loads:
        load.start()

    phase("slots")
    places = lax.broadcasted_iota(jnp.int32, (NZ, LANES), 0)
    experts = (z + away(places) + NZ) % NZ
    hit0, hit1 = experts == routes[0:1, :], experts == routes[1:2, :]
    named = jnp.logical_or(hit0, hit1)
    earlier_than = (
        lax.broadcasted_iota(jnp.int32, (LANES, LANES), 0)
        < lax.broadcasted_iota(jnp.int32, (LANES, LANES), 1)
    ).astype(BF16)
    earlier = dot(named.astype(F32).astype(BF16), earlier_than, (1, 0))
    place = jnp.where(named, earlier, -1.0)
    weight = jnp.where(hit0, weights[0:1, :], 0.0) + jnp.where(hit1, weights[1:2, :], 0.0)
    slot_ids = lax.broadcasted_iota(jnp.int32, (PAD, LANES), 0).astype(F32)
    gains = []
    for j in range(NZ):
        picked = slot_ids == place[j : j + 1, :]
        pall[PAD * j : PAD * (j + 1), :] = picked.astype(F32).astype(BF16)
        gains.append(
            jnp.sum(jnp.where(picked, weight[j : j + 1, :], 0.0), axis=1, keepdims=True)
        )
    pad[...] = jnp.zeros_like(pad)
    home[...] = jnp.zeros_like(home)
    gp[...] = jnp.zeros_like(gp)
    phase("fill")
    loads[0].wait()
    rows = dot(pall[...], tok_v[...], (1, 0)).astype(BF16)
    for j in range(NZ):
        send[0, j] = rows[PAD * j : PAD * j + CAP, :]
    loads[1].wait()
    rows = dot(pall[...], cot_v[...], (1, 0))
    for j in range(NZ):
        send[1, j] = (rows[PAD * j : PAD * j + CAP, :] * gains[j][:CAP, :]).astype(BF16)
    lanes_of = lax.broadcasted_iota(jnp.int32, (HALF, NEAR * PAD), 1)
    slot = lanes_of % PAD
    squeeze = jnp.logical_and(
        lax.broadcasted_iota(jnp.int32, (HALF, NEAR * PAD), 0) == (lanes_of // PAD) * CAP + slot,
        slot < CAP,
    ).astype(F32).astype(BF16)
    for load in loads[2:]:
        load.wait()

    phase("barrier_wait")
    pl.semaphore_wait(barrier, 2 * NZ - 1 + SIDE * SIDE - 1)

    phase("dispatch")
    def to_same(j):
        i = c * NZ + j
        to = (z + away(j) + NZ) % NZ * 2 + c
        return remote(send.at[c, j], recv.at[i], z_send.at[0, j], z_recv.at[i], (to, t))

    def to_other(j):
        i = c * NZ + j
        to = (z + away(j) + NZ) % NZ * 2 + 1 - c
        return remote(send.at[1 - c, j], recv.at[i], z_send.at[1, j], z_recv.at[i], (to, t))

    def dispatch(j, carry):
        to_same(j).start()
        to_other(j).start()
        return carry

    lax.fori_loop(*OTHERS, dispatch, 0)
    to_other(SELF).start()
    recv[c * NZ + SELF] = send[c, SELF]

    waits = []

    def arrived(i):
        remote(recv.at[i], recv.at[i], z_send.at[0, 0], z_recv.at[i], partner).wait_recv()

    def arrive_one(j, carry):
        arrived(j)
        arrived(NZ + j)
        return carry

    def arrive(k):
        first, last = max(k * NEAR, OTHERS[0]), min((k + 1) * NEAR, OTHERS[1])
        lax.fori_loop(first, last, arrive_one, 0)
        if SELF // NEAR == k:
            arrived((1 - c) * NZ + SELF)
        for core in range(2):
            first = core * NZ + k * NEAR
            for i in range(first, first + NEAR):
                pad[PAD * i : PAD * i + CAP, :] = recv[i]
            at = k * PART + core * HALF
            xs[c, at : at + HALF, own_cols] = dot(
                squeeze, pad[PAD * first : PAD * (first + NEAR), :], (1, 0)
            ).astype(BF16)

    WHOLE, LOW, HIGH = (0, PART), (0, HALF), (HALF, HALF)

    def piece(k, o1, o2, part):
        cols = pl.ds(pl.multiple_of(block(o1, o2) * LANES, LANES), LANES)
        return xs.at[c, pl.ds(k * PART + part[0], part[1]), cols]

    def ship(src, dst, send_sem, recv_sem, device):
        copy = remote(src, dst, send_sem, recv_sem, device)
        copy.start()
        waits.append(copy)
        return copy

    def pass_on(k, o1, o2, part, send_sem, recv_sem, device):
        ref = piece(k, o1, o2, part)
        ship(ref, ref, send_sem, recv_sem, device)

    def came(k, o1, o2, part, recv_sem):
        ref = piece(k, o1, o2, part)
        remote(ref, ref, recv_sem, recv_sem, partner).wait_recv()

    def hand_over(k, o1, o2):
        i = (o1 % SIDE) * SIDE + o2 % SIDE
        pass_on(k, o1, o2, WHOLE, ps.at[k, i], pn.at[k, i], partner)

    def both_ways(k, o1):
        j = o1 % SIDE
        pass_on(k, o1, 0, WHOLE, s2.at[k, j, 0], n2.at[k, j, 0], along2(1))
        pass_on(k, o1, 0, WHOLE, s2.at[k, j, 1], n2.at[k, j, 1], along2(-1))

    def gather0(k):
        pass_on(k, 0, 0, WHOLE, s1.at[k, 0], n1.at[k, 0], along1(1))
        pass_on(k, 0, 0, WHOLE, s1.at[k, 1], n1.at[k, 1], along1(-1))
        both_ways(k, 0)
        hand_over(k, 0, 0)

    def gather1(k):
        came(k, -1, 0, WHOLE, n1.at[k, 0])
        pass_on(k, -1, 0, LOW, s1.at[k, 2], n1.at[k, 2], along1(1))
        both_ways(k, -1)
        hand_over(k, -1, 0)
        came(k, 1, 0, WHOLE, n1.at[k, 1])
        pass_on(k, 1, 0, HIGH, s1.at[k, 3], n1.at[k, 3], along1(-1))
        both_ways(k, 1)
        hand_over(k, 1, 0)

    def across(k, o1):
        j = o1 % SIDE
        came(k, o1, -1, WHOLE, n2.at[k, j, 0])
        pass_on(k, o1, -1, LOW, s2.at[k, j, 2], n2.at[k, j, 2], along2(1))
        hand_over(k, o1, -1)
        came(k, o1, 1, WHOLE, n2.at[k, j, 1])
        pass_on(k, o1, 1, HIGH, s2.at[k, j, 3], n2.at[k, j, 3], along2(-1))
        hand_over(k, o1, 1)

    def gather2(k):
        across(k, 0)

    def gather3(k):
        came(k, 2, 0, LOW, n1.at[k, 2])
        came(k, 2, 0, HIGH, n1.at[k, 3])
        both_ways(k, 2)
        hand_over(k, 2, 0)

    def gather4(k):
        across(k, -1)
        across(k, 1)

    def gather5(k):
        across(k, 2)

    def last_of(k, o1):
        j = o1 % SIDE
        came(k, o1, 2, LOW, n2.at[k, j, 2])
        came(k, o1, 2, HIGH, n2.at[k, j, 3])
        hand_over(k, o1, 2)

    def gather6(k):
        for o1 in (0, -1, 1, 2):
            last_of(k, o1)

    def gather7(k):
        for o1 in range(SIDE):
            for o2 in range(SIDE):
                cols = pl.ds(pl.multiple_of(block_of_partner(o1, o2) * LANES, LANES), LANES)
                ref = xs.at[1 - c, pl.ds(k * PART, PART), cols]
                sem = pn.at[k, o1 * SIDE + o2]
                remote(ref, ref, sem, sem, partner).wait_recv()

    combine = {}
    order = (2, 1, 3, 0)

    def expert(k):
        at = slice(k * PART, (k + 1) * PART)
        pre = dot(xs[0, at, :], wgu[...], (1, 0))
        dh = dot(xs[1, at, :], down_v[...], (1, 1))
        a, b = pre[:, :LANES], pre[:, LANES:]
        sigma = jax.nn.sigmoid(a)
        activ = a * sigma
        hidden = activ * b
        dgu[at, :LANES] = (dh * b * sigma * (1.0 + a * (1.0 - sigma))).astype(BF16)
        dgu[at, LANES:] = (dh * activ).astype(BF16)
        hid[at, :] = hidden.astype(BF16)
        part = hidden * dh
        high = part.astype(BF16)
        low = (part - high.astype(F32)).astype(BF16)
        for core in range(2):
            here = slice(core * HALF, (core + 1) * HALF)
            units = dot(high[here, :], squeeze, (0, 0)) + dot(low[here, :], squeeze, (0, 0))
            line = jnp.sum(units, axis=0, keepdims=True)
            for i in range(GATES):
                gp[k, core * GATES + i : core * GATES + i + 1, :] = line[
                    :, LANES * i : LANES * (i + 1)
                ]

    gates = {}

    def gate0(k):
        gates[k] = ship(gp.at[k], gq.at[k], gs.at[k], gn.at[k], partner)

    def gate1(k):
        gates[k].wait_recv()
        gsum[k] = gp[k] + gq[k]
        gates[k] = []
        for i in range(1, SIDE * SIDE):
            to = (ep, block(i // SIDE, i % SIDE))
            gates[k].append(
                ship(gsum.at[k], gall.at[k, i - 1], hs.at[k, i - 1], hn.at[k, i - 1], to)
            )

    def gate2(k):
        for copy in gates[k]:
            copy.wait_recv()
        total = gsum[k]
        for i in range(SIDE * SIDE - 1):
            total = total + gall[k, i]
        gt[k] = total

    def dx_other(k):
        rows_of = pl.ds(pl.multiple_of(k * PART + (1 - c) * HALF, 8), HALF)
        for o1 in order:
            for o2 in range(SIDE):
                units = pl.ds(pl.multiple_of(block_of_partner(o1, o2) * LANES, LANES), LANES)
                dother[k, o1, o2] = dot(dgu[rows_of, :], wgu[units, :], (1, 1)).astype(BF16)
            combine[k, o1] = ship(
                dother.at[k, o1], crecv.at[k, o1], cs.at[k, o1], cn.at[k, o1], partner
            )

    def dx_own(k):
        rows_of = pl.ds(pl.multiple_of(k * PART + c * HALF, 8), HALF)
        for o1 in order:
            for o2 in range(SIDE):
                units = pl.ds(pl.multiple_of(block(o1, o2) * LANES, LANES), LANES)
                dacc[k, o1, o2] = dot(dgu[rows_of, :], wgu[units, :], (1, 1))

    lo, hi = pl.ds(0, CUT), pl.ds(CUT, HALF - CUT)
    flight = {}

    def both(k, o1, part):
        return dacc[k, o1, :, part] + crecv[k, o1, :, part].astype(F32)

    def scatter1(k):
        ss, rr = rs_send.at[k], rs_recv.at[k]
        combine[k, 2].wait_recv()
        rs[k, 2] = (dacc[k, 2] + crecv[k, 2].astype(F32)).astype(BF16)
        flight[k, 0] = ship(
            rs.at[k, 2, :, lo], r1.at[k, 0, :, lo], ss.at[0], rr.at[0], along1(1)
        )
        flight[k, 1] = ship(
            rs.at[k, 2, :, hi], r1.at[k, 1, :, hi], ss.at[1], rr.at[1], along1(-1)
        )
        combine[k, 1].wait_recv()
        rs[k, 1, :, hi] = both(k, 1, hi).astype(BF16)
        flight[k, 2] = ship(
            rs.at[k, 1, :, hi], r2.at[k, 0, :, hi], ss.at[2], rr.at[2], along1(1)
        )
        combine[k, 3].wait_recv()
        rs[k, 3, :, lo] = both(k, 3, lo).astype(BF16)
        flight[k, 3] = ship(
            rs.at[k, 3, :, lo], r2.at[k, 1, :, lo], ss.at[3], rr.at[3], along1(-1)
        )

    def scatter2(k):
        ss, rr = rs_send.at[k], rs_recv.at[k]
        flight[k, 0].wait_recv()
        rs[k, 1, :, lo] = (both(k, 1, lo) + r1[k, 0, :, lo].astype(F32)).astype(BF16)
        flight[k, 4] = ship(
            rs.at[k, 1, :, lo], r2.at[k, 0, :, lo], ss.at[4], rr.at[4], along1(1)
        )
        flight[k, 1].wait_recv()
        rs[k, 3, :, hi] = (both(k, 3, hi) + r1[k, 1, :, hi].astype(F32)).astype(BF16)
        flight[k, 5] = ship(
            rs.at[k, 3, :, hi], r2.at[k, 1, :, hi], ss.at[5], rr.at[5], along1(-1)
        )

    def scatter3(k):
        ss, rr = qs.at[k], qn.at[k]
        combine[k, 0].wait_recv()
        for i in (2, 3, 4, 5):
            flight[k, i].wait_recv()

        def summed(o2):
            return (
                dacc[k, 0, o2] + crecv[k, 0, o2].astype(F32)
                + r2[k, 0, o2].astype(F32) + r2[k, 1, o2].astype(F32)
            )

        send2[k, 2] = summed(2).astype(BF16)
        flight[k, 0] = ship(send2.at[k, 2, lo], q1.at[k, 0, lo], ss.at[0], rr.at[0], along2(1))
        flight[k, 1] = ship(send2.at[k, 2, hi], q1.at[k, 1, hi], ss.at[1], rr.at[1], along2(-1))
        dacc[k, 0, 1] = summed(1)
        send2[k, 1, hi] = dacc[k, 0, 1, hi].astype(BF16)
        flight[k, 2] = ship(send2.at[k, 1, hi], q2.at[k, 0, hi], ss.at[2], rr.at[2], along2(1))
        dacc[k, 0, 3] = summed(3)
        send2[k, 3, lo] = dacc[k, 0, 3, lo].astype(BF16)
        flight[k, 3] = ship(send2.at[k, 3, lo], q2.at[k, 1, lo], ss.at[3], rr.at[3], along2(-1))
        dacc[k, 0, 0] = summed(0)

    def scatter4(k):
        ss, rr = qs.at[k], qn.at[k]
        flight[k, 0].wait_recv()
        send2[k, 1, lo] = (dacc[k, 0, 1, lo] + q1[k, 0, lo].astype(F32)).astype(BF16)
        flight[k, 4] = ship(send2.at[k, 1, lo], q2.at[k, 0, lo], ss.at[4], rr.at[4], along2(1))
        flight[k, 1].wait_recv()
        send2[k, 3, hi] = (dacc[k, 0, 3, hi] + q1[k, 1, hi].astype(F32)).astype(BF16)
        flight[k, 5] = ship(send2.at[k, 3, hi], q2.at[k, 1, hi], ss.at[5], rr.at[5], along2(-1))

    def home_of(j):
        to = (z - away(j) + NZ) % NZ * 2 + c
        return remote(fin.at[j], ret.at[j], fs.at[j], fn.at[j], (to, t))

    def go_home(j, carry):
        home_of(j).start()
        return carry

    def scatter5(k):
        for i in (2, 3, 4, 5):
            flight[k, i].wait_recv()
        total = dacc[k, 0, 0] + q2[k, 0].astype(F32) + q2[k, 1].astype(F32)
        spread = dot(squeeze, total.astype(BF16), (0, 0))
        below = lax.broadcasted_iota(jnp.int32, (PAD, LANES), 0) >= CAP
        for i in range(NEAR):
            r = i * PAD // LANES
            line = jnp.where(c == 0, gt[k, r : r + 1, :], gt[k, GATES + r : GATES + r + 1, :])
            fin[k * NEAR + i] = jnp.where(below, line, spread[PAD * i : PAD * (i + 1), :])[
                :BACK, :
            ].astype(BF16)
        first, last = max(k * NEAR, OTHERS[0]), min((k + 1) * NEAR, OTHERS[1])
        lax.fori_loop(first, last, go_home, 0)
        if SELF // NEAR == k:
            ret[SELF] = fin[SELF]

    def grads(k, carry):
        cols = pl.ds(pl.multiple_of(k * 256, 256), 256)
        part = dot(xs[0, :, cols], dgu[...], (0, 0))
        og[0, cols, :] = part[:, :LANES].astype(BF16)
        ou[0, cols, :] = part[:, LANES:].astype(BF16)
        return carry

    def unit_grads(k):
        lax.fori_loop(0, MODEL // 256, grads, 0)

    def down_grads(k):
        od[0] = dot(hid[...], xs[1], (0, 0)).astype(BF16)

    stages = dict(
        arrive=arrive, gather0=gather0, gather1=gather1, gather2=gather2, gather3=gather3,
        gather4=gather4, gather5=gather5, gather6=gather6, gather7=gather7, expert=expert,
        gate0=gate0, gate1=gate1, gate2=gate2, dx_other=dx_other, dx_own=dx_own,
        scatter1=scatter1, scatter2=scatter2, scatter3=scatter3, scatter4=scatter4,
        scatter5=scatter5, unit_grads=unit_grads, down_grads=down_grads,
    )
    for entry in SCHEDULE:
        phase(entry)
        stages[entry[:-1]](int(entry[-1]))

    phase("rows_came")

    def rows_came(j, carry):
        home_of(j).wait_recv()
        return carry

    lax.fori_loop(*OTHERS, rows_came, 0)
    phase("home")
    for j in range(NZ):
        home[j, :BACK, :] = ret[j]
    flat = home[...].reshape(NZ * PAD, LANES)
    out_tok[...] = dot(pall[...], flat, (0, 0)).astype(BF16)
    at_j = lax.broadcasted_iota(jnp.int32, (NZ, NZ * PAD), 0)
    at_row = lax.broadcasted_iota(jnp.int32, (NZ, NZ * PAD), 1)
    lines = dot((at_row == PAD * at_j + CAP).astype(F32).astype(BF16), flat, (1, 0))
    lines = jnp.concatenate([lines] * (NZ * PAD // LANES), axis=1)
    lines = jnp.where(at_row // PAD == at_j, lines, 0.0).astype(BF16)
    values = dot(lines, pall[...], (1, 0))
    for i, hit in enumerate((hit0, hit1)):
        out_route[i : i + 1, :] = (
            jnp.sum(jnp.where(hit, values, 0.0), axis=0, keepdims=True) / weights[i : i + 1, :]
        )

    phase("drain")
    def drain(j, carry):
        to_same(j).wait_send()
        to_other(j).wait_send()
        home_of(j).wait_send()
        return carry

    lax.fori_loop(*OTHERS, drain, 0)
    to_other(SELF).wait_send()
    for copy in waits:
        copy.wait_send()
    phase(None)


def store(*refs):
    n = len(refs) // 2
    copies = [
        pltpu.make_async_copy(refs[i], refs[n + i], refs[-1].at[i]) for i in range(n)
    ]
    for copy in copies:
        copy.start()
    for copy in copies:
        copy.wait()


def local(tokens, routes, route_weights, out_grad, gate_proj, up_proj, down_proj):
    vmem, hbm = pl.BlockSpec(memory_space=pltpu.VMEM), pl.BlockSpec(memory_space=pl.ANY)
    dma, buf = pltpu.SemaphoreType.DMA, pltpu.VMEM
    quad = (SIDE, HALF, LANES)
    shapes = [
        ((LANES, LANES), BF16),
        ((2, LANES), F32),
        ((1, MODEL, LANES), BF16),
        ((1, MODEL, LANES), BF16),
        ((1, LANES, MODEL), BF16),
    ]
    out = pl.pallas_call(
        kernel,
        out_shape=tuple(pltpu.VMEM(*s) for s in shapes),
        in_specs=[vmem, vmem, hbm, hbm, hbm, hbm, hbm],
        out_specs=[vmem] * 5,
        scratch_shapes=[
            buf((LANES, LANES), BF16),
            buf((LANES, LANES), BF16),
            buf((MODEL, 2 * LANES), BF16),
            buf((LANES, MODEL), BF16),
            buf((NZ * PAD, LANES), BF16),
            buf((2, NZ, CAP, LANES), BF16),
            buf((2 * NZ, CAP, LANES), BF16),
            buf((2 * NZ * PAD, LANES), BF16),
            buf((2, ROWS, MODEL), BF16),
            buf((ROWS, 2 * LANES), BF16),
            buf((ROWS, LANES), BF16),
            buf((CHUNKS, SIDE, *quad), BF16),
            buf((CHUNKS, SIDE, *quad), BF16),
            buf((CHUNKS, SIDE, *quad), F32),
            buf((CHUNKS, SIDE, *quad), BF16),
            buf((CHUNKS, 2, *quad), BF16),
            buf((CHUNKS, 2, *quad), BF16),
            buf((CHUNKS, *quad), BF16),
            buf((CHUNKS, 2, HALF, LANES), BF16),
            buf((CHUNKS, 2, HALF, LANES), BF16),
            buf((NZ, BACK, LANES), BF16),
            buf((NZ, BACK, LANES), BF16),
            buf((NZ, PAD, LANES), BF16),
            buf((CHUNKS, 8, LANES), F32),
            buf((CHUNKS, 8, LANES), F32),
            buf((CHUNKS, 8, LANES), F32),
            buf((CHUNKS, SIDE * SIDE - 1, 8, LANES), F32),
            buf((CHUNKS, 8, LANES), F32),
            dma((5,)),
            dma((2, NZ)),
            dma((2 * NZ,)),
            dma((CHUNKS, 4)),
            dma((CHUNKS, 4)),
            dma((CHUNKS, SIDE, 4)),
            dma((CHUNKS, SIDE, 4)),
            dma((CHUNKS, SIDE * SIDE)),
            dma((CHUNKS, SIDE * SIDE)),
            dma((CHUNKS, SIDE)),
            dma((CHUNKS, SIDE)),
            dma((CHUNKS, 6)),
            dma((CHUNKS, 6)),
            dma((CHUNKS, 6)),
            dma((CHUNKS, 6)),
            dma((NZ,)),
            dma((NZ,)),
            dma((CHUNKS,)),
            dma((CHUNKS,)),
            dma((CHUNKS, SIDE * SIDE - 1)),
            dma((CHUNKS, SIDE * SIDE - 1)),
        ],
        compiler_params=pltpu.CompilerParams(
            collective_id=0, has_side_effects=True, vmem_limit_bytes=56 * 2**20
        ),
        name="routed_backward",
    )(routes.T, route_weights.T, tokens, out_grad, gate_proj, up_proj, down_proj)
    out = pl.pallas_call(
        store,
        out_shape=tuple(jax.ShapeDtypeStruct(*s) for s in shapes),
        in_specs=[vmem] * 5,
        out_specs=[hbm] * 5,
        scratch_shapes=[dma((5,))],
        name="store",
    )(*(pltpu.with_memory_space_constraint(a, pltpu.VMEM) for a in out))
    return (out[0], out[1].T, out[2], out[3], out[4])


SCHEDULE = (
    "arrive0", "gather00", "gather10", "gather20", "gather30", "gather40", "gather50",
    "gather60", "gather70", "expert0", "gate00", "dx_other0", "gate10", "dx_own0", "scatter10",
    "scatter20", "gate20", "scatter30", "scatter40", "scatter50", "unit_grads0", "down_grads0",
)


def solution(mesh):
    placed = (
        P("ep", None),
        P("ep", None),
        P("ep", None),
        P("ep", None),
        P("ep", None, "tp"),
        P("ep", None, "tp"),
        P("ep", "tp", None),
    )
    return jax.shard_map(
        local,
        mesh=mesh,
        in_specs=placed,
        out_specs=(
            P("ep", "tp"),
            P("ep", None),
            P("ep", None, "tp"),
            P("ep", None, "tp"),
            P("ep", "tp", None),
        ),
        check_vma=False,
    )
```

```python
import jax
import jax.numpy as jnp
from jax import lax
from jax.experimental import pallas as pl
from jax.experimental.pallas import tpu as pltpu
from jax.sharding import PartitionSpec as P

MESH = pl.DeviceIdType.MESH
F32, BF16 = jnp.float32, jnp.bfloat16
NZ, SIDE = 16, 4
CAP, PAD, BACK, SENT = 18, 32, 24, 40
LANES = 128
MODEL = 2048
ROWS = 2 * NZ * CAP
CHUNKS = 2
NEAR = NZ // CHUNKS
HALF = NEAR * CAP
PART = 2 * HALF
SELF, OTHERS = NZ - 1, (0, NZ - 1)
DIRECT = (2,)
GATES = NEAR * PAD // LANES


def dot(left, right, dims):
    return lax.dot_general(
        left, right, ((dims[:1], dims[1:]), ((), ())), preferred_element_type=F32
    )


def away(i):
    step = NZ // 2 - (i + 1) // 2
    return step * (2 * (i % 2) - 1)


def kernel(
    routes_hbm, weights_hbm, tok_hbm, cot_hbm, gate_hbm, up_hbm, down_hbm,
    out_tok, out_route, og, ou, od,
    routes, weights, tok_v, cot_v, wgu, wgu_t, down_v, down_t, pall, pdy, send, recv, xs, dgu, hid,
    dother, crecv, dacc, rs, r1, rs2, r2, fin, ret, home, gp, gq, gsum, gall, gt,
    in_sem, z_send, z_recv, s1, n1, s2, n2, ps, pn,
    cs, cn, rs_send, rs_recv, qs, qn, fs, fn, gs, gn, hs, hn,
):
    ep, t = lax.axis_index("ep"), lax.axis_index("tp")
    z, c = ep // 2, ep % 2
    y, x = t // SIDE, t % SIDE
    p1, p2 = x + c * (y - x), y + c * (x - y)
    w1, w2 = 1 + 3 * c, 4 - 3 * c

    def block(o1, o2):
        return w1 * ((p1 + o1) % SIDE) + w2 * ((p2 + o2) % SIDE)

    def block_of_partner(o1, o2):
        return w2 * ((p2 + o1) % SIDE) + w1 * ((p1 + o2) % SIDE)

    def along1(o):
        return (ep, block(o, 0))

    def along2(o):
        return (ep, block(0, o))

    partner = (z * 2 + 1 - c, t)

    def remote(src, dst, send_sem, recv_sem, device):
        return pltpu.make_async_remote_copy(
            src_ref=src, dst_ref=dst, send_sem=send_sem, recv_sem=recv_sem,
            device_id=device, device_id_type=MESH,
        )

    scope = []

    def phase(name):
        if scope:
            scope.pop().__exit__(None, None, None)
        if name:
            scope.append(jax.named_scope(name))
            scope[0].__enter__()

    own_cols = pl.ds(pl.multiple_of(t * LANES, LANES), LANES)
    loads = [
        pltpu.make_async_copy(routes_hbm, routes, in_sem.at[5]),
        pltpu.make_async_copy(weights_hbm, weights, in_sem.at[6]),
        pltpu.make_async_copy(tok_hbm.at[:, own_cols], tok_v, in_sem.at[0]),
        pltpu.make_async_copy(cot_hbm.at[:, own_cols], cot_v, in_sem.at[1]),
        pltpu.make_async_copy(gate_hbm.at[0], wgu.at[:, pl.ds(0, LANES)], in_sem.at[2]),
        pltpu.make_async_copy(up_hbm.at[0], wgu.at[:, pl.ds(LANES, LANES)], in_sem.at[3]),
        pltpu.make_async_copy(down_hbm.at[0], down_v, in_sem.at[4]),
    ]
    for load in loads:
        load.start()

    phase("greet")
    barrier = pltpu.get_barrier_semaphore()

    def greet(i, carry):
        to = ((ep + 2 * i) % (2 * NZ), t)
        pl.semaphore_signal(barrier, inc=1, device_id=to, device_id_type=MESH)
        return carry

    def greet_plane(i, carry):
        to = (ep, (t + i) % (SIDE * SIDE))
        pl.semaphore_signal(barrier, inc=1, device_id=to, device_id_type=MESH)
        return carry

    lax.fori_loop(1, NZ, greet, 0)
    pl.semaphore_signal(barrier, inc=1, device_id=partner, device_id_type=MESH)
    lax.fori_loop(1, SIDE * SIDE, greet_plane, 0)

    phase("slots")
    loads[0].wait()
    loads[1].wait()
    places = lax.broadcasted_iota(jnp.int32, (NZ, LANES), 0)
    experts = (z + away(places) + NZ) % NZ
    hit0, hit1 = experts == routes[0:1, :], experts == routes[1:2, :]
    named = jnp.logical_or(hit0, hit1)
    earlier_than = (
        lax.broadcasted_iota(jnp.int32, (LANES, LANES), 0)
        < lax.broadcasted_iota(jnp.int32, (LANES, LANES), 1)
    ).astype(BF16)
    earlier = dot(named.astype(F32).astype(BF16), earlier_than, (1, 0))
    place = jnp.where(named, earlier, -1.0)
    weight = jnp.where(hit0, weights[0:1, :], 0.0) + jnp.where(hit1, weights[1:2, :], 0.0)
    sent_ids = lax.broadcasted_iota(jnp.int32, (SENT, LANES), 0)
    x_ids = jnp.where(sent_ids < CAP, sent_ids, -2).astype(F32)
    dy_ids = jnp.where(sent_ids >= CAP, sent_ids - CAP, -2).astype(F32)
    gains = []
    for j in range(NZ):
        here = slice(SENT * j, SENT * (j + 1))
        pall[here, :] = (x_ids == place[j : j + 1, :]).astype(F32).astype(BF16)
        picked = dy_ids == place[j : j + 1, :]
        pdy[here, :] = picked.astype(F32).astype(BF16)
        gains.append(
            jnp.sum(jnp.where(picked, weight[j : j + 1, :], 0.0), axis=1, keepdims=True)
        )
    home[...] = jnp.zeros_like(home)
    gp[...] = jnp.zeros_like(gp)
    phase("fill")
    loads[2].wait()
    loads[3].wait()
    x_sent = dot(pall[...], tok_v[...], (1, 0))
    dy_sent = dot(pdy[...], cot_v[...], (1, 0))
    for j in range(NZ):
        here = slice(SENT * j, SENT * (j + 1))
        send[here, :] = (x_sent[here, :] + dy_sent[here, :] * gains[j]).astype(BF16)
    row_of = lax.broadcasted_iota(jnp.int32, (HALF, NEAR * SENT), 0)
    lanes_of = lax.broadcasted_iota(jnp.int32, (HALF, NEAR * SENT), 1)
    from_row = lanes_of % SENT
    at_row = (lanes_of // SENT) * CAP + from_row
    pick_x = jnp.logical_and(row_of == at_row, from_row < CAP).astype(F32).astype(BF16)
    pick_dy = jnp.logical_and(
        row_of == at_row - CAP, jnp.logical_and(from_row >= CAP, from_row < 2 * CAP)
    ).astype(F32).astype(BF16)
    lanes_of = lax.broadcasted_iota(jnp.int32, (HALF, NEAR * PAD), 1)
    slot = lanes_of % PAD
    squeeze = jnp.logical_and(
        lax.broadcasted_iota(jnp.int32, (HALF, NEAR * PAD), 0) == (lanes_of // PAD) * CAP + slot,
        slot < CAP,
    ).astype(F32).astype(BF16)
    phase("barrier_wait")
    pl.semaphore_wait(barrier, NZ + SIDE * SIDE - 1)

    phase("dispatch")
    def sent(j):
        return pl.ds(pl.multiple_of(j * SENT, 8), SENT)

    def to_expert(j):
        to = (z + away(j) + NZ) % NZ * 2 + c
        return remote(send.at[sent(j), :], recv.at[sent(j), :], z_send.at[j], z_recv.at[j], (to, t))

    def dispatch(j, carry):
        to_expert(j).start()
        return carry

    lax.fori_loop(*OTHERS, dispatch, 0)
    recv[SENT * SELF : SENT * (SELF + 1), :] = send[SENT * SELF : SENT * (SELF + 1), :]

    waits = []

    phase("turn")
    for load in loads[4:]:
        load.wait()
    for i in range(SIDE * SIDE):
        at = slice(LANES * i, LANES * (i + 1))
        wgu_t[i] = wgu[at, :].T
        down_t[at, :] = down_v[:, at].T

    def arrive_one(j, carry):
        to_expert(j).wait_recv()
        return carry

    def arrive(k):
        first, last = max(k * NEAR, OTHERS[0]), min((k + 1) * NEAR, OTHERS[1])
        lax.fori_loop(first, last, arrive_one, 0)
        came_in = recv[SENT * NEAR * k : SENT * NEAR * (k + 1), :]
        at = pl.ds(pl.multiple_of(k * PART + c * HALF, 8), HALF)
        xs[0, at, own_cols] = dot(pick_x, came_in, (1, 0)).astype(BF16)
        xs[1, at, own_cols] = dot(pick_dy, came_in, (1, 0)).astype(BF16)

    WHOLE, LOW, HIGH = (0, 2), (0, 1), (1, 1)

    def piece(k, o1, o2, part):
        cols = pl.ds(pl.multiple_of(block(o1, o2) * LANES, LANES), LANES)
        at = pl.ds(pl.multiple_of(k * PART + c * HALF, 8), HALF)
        return xs.at[pl.ds(*part), at, cols]

    def ship(src, dst, send_sem, recv_sem, device):
        copy = remote(src, dst, send_sem, recv_sem, device)
        copy.start()
        waits.append(copy)
        return copy

    def pass_on(k, o1, o2, part, send_sem, recv_sem, device):
        ref = piece(k, o1, o2, part)
        ship(ref, ref, send_sem, recv_sem, device)

    def came(k, o1, o2, part, recv_sem):
        ref = piece(k, o1, o2, part)
        remote(ref, ref, recv_sem, recv_sem, partner).wait_recv()

    def hand_over(k, o1, o2):
        i = (o1 % SIDE) * SIDE + o2 % SIDE
        pass_on(k, o1, o2, WHOLE, ps.at[k, i], pn.at[k, i], partner)

    def both_ways(k, o1):
        j = o1 % SIDE
        pass_on(k, o1, 0, WHOLE, s2.at[k, j, 0], n2.at[k, j, 0], along2(1))
        pass_on(k, o1, 0, WHOLE, s2.at[k, j, 1], n2.at[k, j, 1], along2(-1))
        if j in DIRECT:
            pass_on(k, o1, 0, WHOLE, s2.at[k, j, 2], n2.at[k, j, 2], along2(2))

    def gather0(k):
        pass_on(k, 0, 0, WHOLE, s1.at[k, 0], n1.at[k, 0], along1(1))
        pass_on(k, 0, 0, WHOLE, s1.at[k, 1], n1.at[k, 1], along1(-1))
        pass_on(k, 0, 0, WHOLE, s1.at[k, 2], n1.at[k, 2], along1(2))
        both_ways(k, 0)
        hand_over(k, 0, 0)

    def gather1(k):
        came(k, -1, 0, WHOLE, n1.at[k, 0])
        both_ways(k, -1)
        hand_over(k, -1, 0)
        came(k, 1, 0, WHOLE, n1.at[k, 1])
        both_ways(k, 1)
        hand_over(k, 1, 0)

    def across(k, o1):
        j = o1 % SIDE
        came(k, o1, -1, WHOLE, n2.at[k, j, 0])
        if j not in DIRECT:
            pass_on(k, o1, -1, LOW, s2.at[k, j, 2], n2.at[k, j, 2], along2(1))
        hand_over(k, o1, -1)
        came(k, o1, 1, WHOLE, n2.at[k, j, 1])
        if j not in DIRECT:
            pass_on(k, o1, 1, HIGH, s2.at[k, j, 3], n2.at[k, j, 3], along2(-1))
        hand_over(k, o1, 1)

    def gather2(k):
        across(k, 0)

    def gather3(k):
        came(k, 2, 0, WHOLE, n1.at[k, 2])
        both_ways(k, 2)
        hand_over(k, 2, 0)

    def gather4(k):
        across(k, -1)
        across(k, 1)

    def gather5(k):
        across(k, 2)

    def last_of(k, o1):
        j = o1 % SIDE
        if j in DIRECT:
            came(k, o1, 2, WHOLE, n2.at[k, j, 2])
        else:
            came(k, o1, 2, LOW, n2.at[k, j, 2])
            came(k, o1, 2, HIGH, n2.at[k, j, 3])
        hand_over(k, o1, 2)

    def gather6(k):
        for o1 in (0, -1, 1, 2):
            last_of(k, o1)

    def gather7(k):
        for o1 in range(SIDE):
            for o2 in range(SIDE):
                cols = pl.ds(pl.multiple_of(block_of_partner(o1, o2) * LANES, LANES), LANES)
                at = pl.ds(pl.multiple_of(k * PART + (1 - c) * HALF, 8), HALF)
                ref = xs.at[:, at, cols]
                sem = pn.at[k, o1 * SIDE + o2]
                remote(ref, ref, sem, sem, partner).wait_recv()

    combine = {}
    order = (2, 1, 3, 0)

    def expert(k):
        at = slice(k * PART, (k + 1) * PART)
        pre = dot(xs[0, at, :], wgu[...], (1, 0))
        dh = dot(xs[1, at, :], down_t[...], (1, 0))
        a, b = pre[:, :LANES], pre[:, LANES:]
        sigma = jax.nn.sigmoid(a)
        activ = a * sigma
        hidden = activ * b
        dgu[at, :LANES] = (dh * b * sigma * (1.0 + a * (1.0 - sigma))).astype(BF16)
        dgu[at, LANES:] = (dh * activ).astype(BF16)
        hid[at, :] = hidden.astype(BF16)
        part = hidden * dh
        high = part.astype(BF16)
        low = (part - high.astype(F32)).astype(BF16)
        for core in range(2):
            here = slice(core * HALF, (core + 1) * HALF)
            units = dot(high[here, :], squeeze, (0, 0)) + dot(low[here, :], squeeze, (0, 0))
            line = jnp.sum(units, axis=0, keepdims=True)
            for i in range(GATES):
                gp[k, core * GATES + i : core * GATES + i + 1, :] = line[
                    :, LANES * i : LANES * (i + 1)
                ]

    gates = {}

    def gate0(k):
        gates[k] = ship(gp.at[k], gq.at[k], gs.at[k], gn.at[k], partner)

    def gate1(k):
        gates[k].wait_recv()
        gsum[k] = gp[k] + gq[k]
        gates[k] = []
        for i in range(1, SIDE * SIDE):
            to = (ep, block(i // SIDE, i % SIDE))
            gates[k].append(
                ship(gsum.at[k], gall.at[k, i - 1], hs.at[k, i - 1], hn.at[k, i - 1], to)
            )

    def gate2(k):
        for copy in gates[k]:
            copy.wait_recv()
        total = gsum[k]
        for i in range(SIDE * SIDE - 1):
            total = total + gall[k, i]
        gt[k] = total

    def dx_other(k):
        rows_of = pl.ds(pl.multiple_of(k * PART + (1 - c) * HALF, 8), HALF)
        for o1 in order:
            for o2 in range(SIDE):
                units = wgu_t[block_of_partner(o1, o2)]
                dother[k, o1, o2] = dot(dgu[rows_of, :], units, (1, 0)).astype(BF16)
            combine[k, o1] = ship(
                dother.at[k, o1], crecv.at[k, o1], cs.at[k, o1], cn.at[k, o1], partner
            )

    def partial(k, o1, o2):
        rows_of = pl.ds(pl.multiple_of(k * PART + c * HALF, 8), HALF)
        return dot(dgu[rows_of, :], wgu_t[block(o1, o2)], (1, 0))

    flight = {}

    def scatter1(k):
        for o1 in order:
            for o2 in range(SIDE):
                dacc[k, o1, o2] = partial(k, o1, o2)
            if o1:
                combine[k, o1].wait_recv()
                rs[k, o1] = (dacc[k, o1] + crecv[k, o1].astype(F32)).astype(BF16)
                flight[k, o1] = ship(
                    rs.at[k, o1], r1.at[k, o1 - 1], rs_send.at[k, o1], rs_recv.at[k, o1], along1(o1)
                )

    def scatter2(k):
        combine[k, 0].wait_recv()
        for o1 in (1, 3, 2):
            flight[k, o1].wait_recv()
        for o2 in order:
            total = (
                dacc[k, 0, o2] + crecv[k, 0, o2].astype(F32)
                + r1[k, 0, o2].astype(F32) + r1[k, 1, o2].astype(F32) + r1[k, 2, o2].astype(F32)
            )
            if o2:
                rs2[k, o2] = total.astype(BF16)
                flight[k, o2] = ship(
                    rs2.at[k, o2], r2.at[k, o2 - 1], qs.at[k, o2], qn.at[k, o2], along2(o2)
                )
            else:
                dacc[k, 0, 0] = total

    def home_of(j):
        to = (z - away(j) + NZ) % NZ * 2 + c
        return remote(fin.at[j], ret.at[j], fs.at[j], fn.at[j], (to, t))

    def go_home(j, carry):
        home_of(j).start()
        return carry

    def scatter3(k):
        for o2 in (1, 3, 2):
            flight[k, o2].wait_recv()
        total = (
            dacc[k, 0, 0] + r2[k, 0].astype(F32) + r2[k, 1].astype(F32) + r2[k, 2].astype(F32)
        )
        spread = dot(squeeze, total.astype(BF16), (0, 0))
        below = lax.broadcasted_iota(jnp.int32, (PAD, LANES), 0) >= CAP
        for i in range(NEAR):
            r = i * PAD // LANES
            line = jnp.where(c == 0, gt[k, r : r + 1, :], gt[k, GATES + r : GATES + r + 1, :])
            fin[k * NEAR + i] = jnp.where(below, line, spread[PAD * i : PAD * (i + 1), :])[
                :BACK, :
            ].astype(BF16)
        first, last = max(k * NEAR, OTHERS[0]), min((k + 1) * NEAR, OTHERS[1])
        lax.fori_loop(first, last, go_home, 0)
        if SELF // NEAR == k:
            ret[SELF] = fin[SELF]

    def grads(k, carry):
        cols = pl.ds(pl.multiple_of(k * 256, 256), 256)
        part = dot(xs[0, :, cols], dgu[...], (0, 0))
        og[0, cols, :] = part[:, :LANES].astype(BF16)
        ou[0, cols, :] = part[:, LANES:].astype(BF16)
        return carry

    def unit_grads(k):
        lax.fori_loop(0, MODEL // 256, grads, 0)

    def down_grads(k):
        od[0] = dot(hid[...], xs[1], (0, 0)).astype(BF16)

    stages = dict(
        arrive=arrive, gather0=gather0, gather1=gather1, gather2=gather2, gather3=gather3,
        gather4=gather4, gather5=gather5, gather6=gather6, gather7=gather7, expert=expert,
        gate0=gate0, gate1=gate1, gate2=gate2, dx_other=dx_other, scatter1=scatter1,
        scatter2=scatter2, scatter3=scatter3, unit_grads=unit_grads, down_grads=down_grads,
    )
    for entry in SCHEDULE:
        phase(entry)
        stages[entry[:-1]](int(entry[-1]))

    phase("rows_came")

    def rows_came(j, carry):
        home_of(j).wait_recv()
        return carry

    lax.fori_loop(*OTHERS, rows_came, 0)
    phase("home")
    for j in range(NZ):
        home[j, :BACK, :] = ret[j]
    flat = home[...].reshape(NZ * SENT, LANES)
    out_tok[...] = dot(pall[...], flat, (0, 0)).astype(BF16)
    at_j = lax.broadcasted_iota(jnp.int32, (NZ, NZ * SENT), 0)
    at_row = lax.broadcasted_iota(jnp.int32, (NZ, NZ * SENT), 1)
    lines = dot((at_row == SENT * at_j + CAP).astype(F32).astype(BF16), flat, (1, 0))
    values = jnp.zeros((NZ, LANES), F32)
    lanes_of = lax.broadcasted_iota(jnp.int32, (NZ, LANES), 1)
    by_slot = jnp.zeros((NZ, PAD), F32)
    for i in range(LANES // PAD):
        mine = lax.broadcasted_iota(jnp.int32, (NZ, PAD), 0) % (LANES // PAD) == i
        by_slot = by_slot + jnp.where(mine, lines[:, PAD * i : PAD * (i + 1)], 0.0)
    by_slot = by_slot.astype(BF16)
    for j in range(NZ):
        mine = dot(by_slot, pall[SENT * j : SENT * j + PAD, :], (1, 0))
        values = jnp.where(lax.broadcasted_iota(jnp.int32, (NZ, LANES), 0) == j, mine, values)
    for i, hit in enumerate((hit0, hit1)):
        out_route[i : i + 1, :] = (
            jnp.sum(jnp.where(hit, values, 0.0), axis=0, keepdims=True) / weights[i : i + 1, :]
        )

    phase("drain")
    def drain(j, carry):
        to_expert(j).wait_send()
        home_of(j).wait_send()
        return carry

    lax.fori_loop(*OTHERS, drain, 0)
    for copy in waits:
        copy.wait_send()
    phase(None)


def store(*refs):
    n = len(refs) // 2
    copies = [
        pltpu.make_async_copy(refs[i], refs[n + i], refs[-1].at[i]) for i in range(n)
    ]
    for copy in copies:
        copy.start()
    for copy in copies:
        copy.wait()


def local(tokens, routes, route_weights, out_grad, gate_proj, up_proj, down_proj):
    vmem, hbm = pl.BlockSpec(memory_space=pltpu.VMEM), pl.BlockSpec(memory_space=pl.ANY)
    dma, buf = pltpu.SemaphoreType.DMA, pltpu.VMEM
    quad = (SIDE, HALF, LANES)
    shapes = [
        ((LANES, LANES), BF16),
        ((2, LANES), F32),
        ((1, MODEL, LANES), BF16),
        ((1, MODEL, LANES), BF16),
        ((1, LANES, MODEL), BF16),
    ]
    out = pl.pallas_call(
        kernel,
        out_shape=tuple(pltpu.VMEM(*s) for s in shapes),
        in_specs=[hbm] * 7,
        out_specs=[vmem] * 5,
        scratch_shapes=[
            buf((2, LANES), jnp.int32),
            buf((2, LANES), F32),
            buf((LANES, LANES), BF16),
            buf((LANES, LANES), BF16),
            buf((MODEL, 2 * LANES), BF16),
            buf((SIDE * SIDE, 2 * LANES, LANES), BF16),
            buf((LANES, MODEL), BF16),
            buf((MODEL, LANES), BF16),
            buf((NZ * SENT, LANES), BF16),
            buf((NZ * SENT, LANES), BF16),
            buf((NZ * SENT, LANES), BF16),
            buf((NZ * SENT, LANES), BF16),
            buf((2, ROWS, MODEL), BF16),
            buf((ROWS, 2 * LANES), BF16),
            buf((ROWS, LANES), BF16),
            buf((CHUNKS, SIDE, *quad), BF16),
            buf((CHUNKS, SIDE, *quad), BF16),
            buf((CHUNKS, SIDE, *quad), F32),
            buf((CHUNKS, SIDE, *quad), BF16),
            buf((CHUNKS, 3, *quad), BF16),
            buf((CHUNKS, *quad), BF16),
            buf((CHUNKS, 3, HALF, LANES), BF16),
            buf((NZ, BACK, LANES), BF16),
            buf((NZ, BACK, LANES), BF16),
            buf((NZ, SENT, LANES), BF16),
            buf((CHUNKS, 8, LANES), F32),
            buf((CHUNKS, 8, LANES), F32),
            buf((CHUNKS, 8, LANES), F32),
            buf((CHUNKS, SIDE * SIDE - 1, 8, LANES), F32),
            buf((CHUNKS, 8, LANES), F32),
            dma((7,)),
            dma((NZ,)),
            dma((NZ,)),
            dma((CHUNKS, 4)),
            dma((CHUNKS, 4)),
            dma((CHUNKS, SIDE, 4)),
            dma((CHUNKS, SIDE, 4)),
            dma((CHUNKS, SIDE * SIDE)),
            dma((CHUNKS, SIDE * SIDE)),
            dma((CHUNKS, SIDE)),
            dma((CHUNKS, SIDE)),
            dma((CHUNKS, SIDE)),
            dma((CHUNKS, SIDE)),
            dma((CHUNKS, SIDE)),
            dma((CHUNKS, SIDE)),
            dma((NZ,)),
            dma((NZ,)),
            dma((CHUNKS,)),
            dma((CHUNKS,)),
            dma((CHUNKS, SIDE * SIDE - 1)),
            dma((CHUNKS, SIDE * SIDE - 1)),
        ],
        compiler_params=pltpu.CompilerParams(
            collective_id=0, has_side_effects=True, vmem_limit_bytes=56 * 2**20
        ),
        name="routed_backward",
    )(routes.T, route_weights.T, tokens, out_grad, gate_proj, up_proj, down_proj)
    out = pl.pallas_call(
        store,
        out_shape=tuple(jax.ShapeDtypeStruct(*s) for s in shapes),
        in_specs=[vmem] * 5,
        out_specs=[hbm] * 5,
        scratch_shapes=[dma((5,))],
        name="store",
    )(*(pltpu.with_memory_space_constraint(a, pltpu.VMEM) for a in out))
    return (out[0], out[1].T, out[2], out[3], out[4])


SCHEDULE = (
    "arrive0", "gather00", "gather10", "gather20", "gather30", "arrive1", "gather01", "gather40",
    "gather11", "gather50", "gather60", "gather21", "gather70", "gather31", "expert0", "gate00",
    "gather41", "dx_other0", "gate10", "gather51", "scatter10", "gather61", "gather71",
    "expert1", "gate01", "dx_other1", "gate11", "scatter20", "scatter11", "gate20", "scatter30",
    "scatter21", "gate21", "scatter31", "unit_grads0", "down_grads0",
)


def solution(mesh):
    placed = (
        P("ep", None),
        P("ep", None),
        P("ep", None),
        P("ep", None),
        P("ep", None, "tp"),
        P("ep", None, "tp"),
        P("ep", "tp", None),
    )
    return jax.shard_map(
        local,
        mesh=mesh,
        in_specs=placed,
        out_specs=(
            P("ep", "tp"),
            P("ep", None),
            P("ep", None, "tp"),
            P("ep", None, "tp"),
            P("ep", "tp", None),
        ),
        check_vma=False,
    )
```
